32 devices in a mesh: grp: 2 (over x), ra: 4 (over z), cb: 4 (over y, core).
Axes of the slice: x: 2, y: 2, z: 4, core: 2. Of those that a mesh axis runs over, the one named last changes fastest.
Arguments:
- tokens: bfloat16 [256, 4096], P('grp', 'ra'), parts along dimension 0, may hold values from -30 to 30
- in_gain: float32 [4096], P('ra'), may hold values from 0.1 to 1.9
- gate_weight: float32 [4096, 11264], P('ra', 'cb'), may hold values from -0.09375 to 0.09375
- gate_scale: float32 [11264], P('cb'), may hold values from 0.3 to 3
- up_weight: float32 [4096, 11264], P('ra', 'cb'), may hold values from -0.09375 to 0.09375
- up_scale: float32 [11264], P('cb'), may hold values from 0.3 to 3
- down_weight: float32 [11264, 4096], P('cb', 'ra'), may hold values from -0.0546875 to 0.0546875
- down_scale: float32 [4096], P('ra'), may hold values from 0.3 to 3
- out_gain: float32 [4096], P('ra'), may hold values from 0.1 to 1.9
Outputs:
- result: bfloat16 [256, 4096], P('grp', 'ra'), parts along dimension 0
The draws below stay inside these ranges and needn't reach their ends.
There are 2 independent parts, one for each index of `grp`. The reference program is written for one: setup_inputs(seed, part) draws one part's arguments, and reference() takes and returns one part's arrays. A program takes and returns all parts, laid end to end along the dimension named above; an argument that names none is the same for every part. Nothing has to cross between parts.
All inputs are finite; a program needn't handle non-finite values.
Results may differ from the reference program's by a relative error of at most 0.008.
Values may be sent and summed in bfloat16 or wider, within the bound.
A program may use at most 64 MiB of HBM per device.

```python
import math
import jax
import jax.numpy as jnp
from jax import lax

D = 4096
FF = 11264
TOK = 128


def draw_tokens(key, part):
    keys = jax.random.split(jax.random.fold_in(key, 11), 2)
    column = jnp.exp(math.log(10.0) * jnp.arange(D, dtype=jnp.float32) / (D - 1))
    rows = jnp.exp(jax.random.uniform(keys[0], (TOK, 1), jnp.float32, 0.0, math.log(10.0)))
    base = jax.random.normal(keys[1], (TOK, D), jnp.float32)
    values = base * rows * column[None, :]
    values = values / jnp.sqrt(jnp.mean(values * values))
    return jnp.clip(values, -30.0, 30.0).astype(jnp.bfloat16)


def levels(key, dims, cuts, low, high):
    gain, own = 1.0, jax.random.fold_in(key, 6)
    for axis_at, blocks in cuts:
        draws = jnp.exp(jax.random.uniform(jax.random.fold_in(own, axis_at), (blocks,), jnp.float32, low / len(cuts), high / len(cuts)))
        gain = gain * jnp.repeat(draws, dims[axis_at] // blocks).reshape([-1 if axis == axis_at else 1 for axis in range(len(dims))])
    return gain


def bell_draw(rng, extent, spread, most, pieces=(), kind=jnp.bfloat16):
    gain = levels(rng, extent, pieces, -0.22, 0.18) if pieces else 1.0
    drawn = jax.random.normal(rng, extent, jnp.float32) * spread * gain
    return jnp.minimum(jnp.maximum(drawn, -most), most).astype(kind)


def setup_inputs(seed: int = 0, part: int = 0) -> dict:
    arg_keys = jax.random.split(jax.random.key(seed), 10)
    own_keys = jax.random.split(jax.random.fold_in(arg_keys[9], part), 10)
    return {
        "tokens": draw_tokens(jax.random.fold_in(jax.random.fold_in(arg_keys[9], part), 71), part),
        "in_gain": jnp.clip(1.0 + 0.18 * jax.random.normal(arg_keys[1], (D,), jnp.float32), 0.1, 1.9),
        "gate_weight": bell_draw(arg_keys[2], (D, FF), D ** -0.5, 0.09375, ((0, 4), (1, 4)), jnp.float32),
        "gate_scale": jnp.clip(jnp.exp(math.log(3.0) - 2.3025851 * jax.random.uniform(arg_keys[3], (FF,), jnp.float32) ** levels(arg_keys[3], (FF,), ((0, 4),), -0.2, 0.2)), 0.3, 3.0),
        "up_weight": bell_draw(arg_keys[4], (D, FF), D ** -0.5, 0.09375, ((0, 4), (1, 4)), jnp.float32),
        "up_scale": jnp.clip(jnp.exp(math.log(3.0) - 2.3025851 * jax.random.uniform(arg_keys[5], (FF,), jnp.float32) ** levels(arg_keys[5], (FF,), ((0, 4),), -0.2, 0.2)), 0.3, 3.0),
        "down_weight": bell_draw(arg_keys[6], (FF, D), FF ** -0.5, 0.0546875, ((0, 4), (1, 4)), jnp.float32),
        "down_scale": jnp.clip(jnp.exp(math.log(3.0) - 2.3025851 * jax.random.uniform(arg_keys[7], (D,), jnp.float32) ** levels(arg_keys[7], (D,), ((0, 4),), -0.2, 0.2)), 0.3, 3.0),
        "out_gain": jnp.clip(1.0 + 0.18 * jax.random.normal(arg_keys[8], (D,), jnp.float32), 0.1, 1.9),
    }


EPSILON = 1e-06
RESIDUAL = 0.5

def reference(tokens, in_gain, gate_weight, gate_scale, up_weight, up_scale, down_weight, down_scale, out_gain):
    tok_float = tokens.astype(jnp.float32)
    inv_rows = lax.rsqrt(lax.optimization_barrier(jnp.mean(tok_float * tok_float, axis=1, keepdims=True)) + EPSILON)
    scaled = (tok_float * in_gain[None, :]).astype(jnp.bfloat16)
    gate_full = jnp.dot(scaled, gate_weight.astype(jnp.bfloat16), preferred_element_type=jnp.float32) * inv_rows * gate_scale[None, :]
    up_full = jnp.dot(scaled, up_weight.astype(jnp.bfloat16), preferred_element_type=jnp.float32) * inv_rows * up_scale[None, :]
    hidden = (jax.nn.silu(gate_full) * up_full).astype(jnp.bfloat16)
    down_full = jnp.dot(hidden, down_weight.astype(jnp.bfloat16), preferred_element_type=jnp.float32)
    mixed_rows = RESIDUAL * tok_float + down_full * down_scale[None, :]
    inv_out = lax.rsqrt(lax.optimization_barrier(jnp.mean(mixed_rows * mixed_rows, axis=1, keepdims=True)) + EPSILON)
    return (mixed_rows * inv_out * out_gain[None, :]).astype(jnp.bfloat16)
```

```python
import functools
import jax
import jax.numpy as jnp
from jax import lax
from jax.experimental import pallas as pl
from jax.experimental.pallas import tpu as pltpu
from jax.sharding import PartitionSpec as P

EPSILON = 1e-06
RESIDUAL = 0.5


def local(
    tokens, in_gain, gate_weight, gate_scale, up_weight, up_scale, down_weight, down_scale, out_gain
):
    tok_float = tokens.astype(jnp.float32)
    local_squares = jnp.sum(tok_float * tok_float, axis=1)
    scaled = (tok_float * in_gain[None, :]).astype(jnp.bfloat16)
    gate_part = jnp.dot(
        scaled, gate_weight.astype(jnp.bfloat16), preferred_element_type=jnp.float32
    )
    up_part = jnp.dot(scaled, up_weight.astype(jnp.bfloat16), preferred_element_type=jnp.float32)
    features = tokens.shape[1] * lax.axis_size("ra")
    gate_sum, up_sum, share_squares = (
        lax.psum_scatter(gate_part, "ra", scatter_dimension=0, tiled=True),
        lax.psum_scatter(up_part, "ra", scatter_dimension=0, tiled=True),
        lax.psum_scatter(local_squares, "ra", scatter_dimension=0, tiled=True),
    )
    inv_rows = lax.rsqrt(share_squares / features + EPSILON)[:, None]
    gate_share = gate_sum * inv_rows * gate_scale[None, :]
    up_share = up_sum * inv_rows * up_scale[None, :]
    hidden_share = (jax.nn.silu(gate_share) * up_share).astype(jnp.bfloat16)
    hidden = lax.all_gather(hidden_share, "ra", axis=0, tiled=True)
    down_part = jnp.dot(
        hidden, down_weight.astype(jnp.bfloat16), preferred_element_type=jnp.float32
    )
    down_full = lax.psum(down_part, "cb")
    mixed_rows = RESIDUAL * tok_float + down_full * down_scale[None, :]
    out_total = lax.psum(jnp.sum(mixed_rows * mixed_rows, axis=1), "ra")
    inv_out = lax.rsqrt(out_total / features + EPSILON)[:, None]
    return (mixed_rows * inv_out * out_gain[None, :]).astype(jnp.bfloat16)


MESH = pl.DeviceIdType.MESH
WIDTH = 256
LAG = 2


def kernel(
    n,
    tok_hbm, gain_hbm, gate_hbm, gscale_hbm, up_hbm, uscale_hbm, down_hbm, dscale_hbm, ogain_hbm,
    out_ref,
    tok, gain, gate, gscale, up, uscale, down, dscale, ogain,
    scaled, part, sent, got, hidden, acc, spread, sq_own, sq_got, inv, half_sent, half_got,
    y_sent, y_got, mixed, out_own, out_got,
    small_sem, gate_sem, up_sem, down_sem, rs_send, rs_recv, ag_send, ag_recv,
    sq_send, sq_recv, half_sem, y_sem, mix_sem, out_send, out_recv,
):
    chunks, half = gate.shape[0], tok.shape[0] // 2
    rows = 2 * half
    features = tok.shape[1] * n
    z, cb = lax.axis_index("ra"), lax.axis_index("cb")
    core = lax.rem(cb, 2)
    mate = cb + 1 - 2 * core
    across = lax.rem(cb + 2, 4)
    right, left = lax.rem(z + 1, n), lax.rem(z + n - 1, n)

    smalls = [
        pltpu.make_async_copy(src, dst, small_sem.at[i])
        for i, (src, dst) in enumerate([
            (tok_hbm, tok), (gain_hbm, gain), (gscale_hbm, gscale),
            (uscale_hbm, uscale), (dscale_hbm, dscale), (ogain_hbm, ogain),
        ])
    ]

    def gate_copy(j):
        cols = pl.ds(pl.multiple_of(j * WIDTH, WIDTH), WIDTH)
        return pltpu.make_async_copy(gate_hbm.at[:, cols], gate.at[j], gate_sem.at[j])

    def up_copy(j):
        cols = pl.ds(pl.multiple_of(j * WIDTH, WIDTH), WIDTH)
        return pltpu.make_async_copy(up_hbm.at[:, cols], up.at[j], up_sem.at[j])

    def down_copy(j):
        at = pl.ds(pl.multiple_of(j * WIDTH, WIDTH), WIDTH)
        return pltpu.make_async_copy(down_hbm.at[at, :], down.at[j], down_sem.at[j])

    for copy in smalls:
        copy.start()
    for j in range(chunks):
        gate_copy(j).start()
        up_copy(j).start()
    for j in range(chunks):
        down_copy(j).start()

    barrier = pltpu.get_barrier_semaphore()
    for step in range(1, n):
        for who in (cb, mate):
            pl.semaphore_signal(barrier, inc=1, device_id={"ra": lax.rem(z + step, n), "cb": who}, device_id_type=MESH)
    for who in (mate, across):
        pl.semaphore_signal(barrier, inc=1, device_id={"cb": who}, device_id_type=MESH)

    for copy in smalls:
        copy.wait()
    tok_float = tok[...].astype(jnp.float32)
    scaled[...] = (tok_float * gain[...]).astype(jnp.bfloat16)
    squares = jnp.sum(tok_float * tok_float, axis=1, keepdims=True)
    spread[...] = jnp.broadcast_to(squares, (rows, 128))
    sq_own[0] = spread[...].T[:8]

    pl.semaphore_wait(barrier, 2 * (n - 1) + 2)

    def sq_copy(step, goal):
        return pltpu.make_async_remote_copy(
            sq_own.at[0], sq_got.at[step - 1], sq_send.at[goal], sq_recv.at[step - 1],
            device_id={"ra": lax.rem(z + step, n)}, device_id_type=MESH,
        )

    for goal, end in enumerate((0, n - 1)):
        for step in range(1, n):
            @pl.when(lax.rem(z + step, n) == end)
            def _():
                sq_copy(step, goal).start()

    def rs_copy(j, side):
        return pltpu.make_async_remote_copy(
            sent.at[side, j], got.at[side, j], rs_send.at[side, j], rs_recv.at[side, j],
            device_id={"ra": right if side else left}, device_id_type=MESH,
        )

    def ag_copy(j, side):
        ref = hidden.at[j, pl.ds(side * half, half)]
        return pltpu.make_async_remote_copy(
            ref, ref, ag_send.at[side, j], ag_recv.at[side, j],
            device_id={"ra": left if side else right}, device_id_type=MESH,
        )

    def rs_step(t, side):
        place = z if side else n - 1 - z
        j = t - LAG * place
        own = pl.ds(side * half, half)

        @pl.when((j >= 0) & (j < chunks))
        def _():
            @pl.when(place == 0)
            def _():
                sent[side, j] = part[j, own].astype(jnp.bfloat16)
                rs_copy(j, side).start()

            @pl.when((place > 0) & (place < n - 1))
            def _():
                rs_copy(j, side).wait_recv()
                sent[side, j] = (part[j, own] + got[side, j].astype(jnp.float32)).astype(jnp.bfloat16)
                rs_copy(j, side).start()

            @pl.when(place == n - 1)
            def _():
                @pl.when(j == 0)
                def _():
                    for step in range(1, n):
                        sq_copy(step, 0).wait_recv()
                    total = sq_own[0] + sq_got[0]
                    for step in range(2, n):
                        total = total + sq_got[step - 1]
                    spread[...] = jnp.broadcast_to(total[:1], (128, 128)).T
                    inv[...] = lax.rsqrt(spread[...] / features + EPSILON)

                rs_copy(j, side).wait_recv()
                cols = pl.ds(pl.multiple_of(j * WIDTH, WIDTH), WIDTH)
                scale = inv[own][:, :1]
                total = part[j, own] + got[side, j].astype(jnp.float32)
                gate_share = total[:, :WIDTH] * scale * gscale[:, cols]
                up_share = total[:, WIDTH:] * scale * uscale[:, cols]
                hidden[j, own] = (jax.nn.silu(gate_share) * up_share).astype(jnp.bfloat16)
                ag_copy(j, side).start()

    def rs_loop(t, carry):
        @pl.when(t < chunks)
        def _():
            gate_copy(t).wait()
            part[t, :, :WIDTH] = jnp.dot(scaled[...], gate[t].astype(jnp.bfloat16), preferred_element_type=jnp.float32)
            up_copy(t).wait()
            part[t, :, WIDTH:] = jnp.dot(scaled[...], up[t].astype(jnp.bfloat16), preferred_element_type=jnp.float32)

        rs_step(t, 0)
        rs_step(t, 1)
        return carry

    lax.fori_loop(0, chunks + LAG * (n - 1), rs_loop, 0)

    def ag_step(u, side):
        place = n - 1 - z if side else z
        j = u - LAG * (place - 1)

        @pl.when((place > 0) & (j >= 0) & (j < chunks))
        def _():
            ag_copy(j, side).wait_recv()

            @pl.when(place < n - 1)
            def _():
                ag_copy(j, side).start()

    acc[...] = jnp.zeros_like(acc)

    def ag_loop(u, carry):
        ag_step(u, 0)
        ag_step(u, 1)
        j = u - LAG * (lax.max(z, n - 1 - z) - 1)

        @pl.when((j >= 0) & (j < chunks))
        def _():
            down_copy(j).wait()
            acc[...] += jnp.dot(hidden[j], down[j].astype(jnp.bfloat16), preferred_element_type=jnp.float32)

        return carry

    lax.fori_loop(0, chunks + LAG * (n - 2), ag_loop, 0)

    mine = pl.ds(pl.multiple_of(core * half, half), half)
    theirs = pl.ds(pl.multiple_of((1 - core) * half, half), half)
    half_sent[...] = acc[theirs].astype(jnp.bfloat16)
    half_copy = pltpu.make_async_remote_copy(
        half_sent, half_got, half_sem.at[0], half_sem.at[1], device_id={"cb": mate}, device_id_type=MESH
    )
    half_copy.start()
    half_copy.wait()
    y_sent[...] = (acc[mine] + half_got[...].astype(jnp.float32)).astype(jnp.bfloat16)
    y_copy = pltpu.make_async_remote_copy(
        y_sent, y_got, y_sem.at[0], y_sem.at[1], device_id={"cb": across}, device_id_type=MESH
    )
    y_copy.start()
    y_copy.wait()
    summed = y_sent[...].astype(jnp.float32) + y_got[...].astype(jnp.float32)
    mixed[0] = RESIDUAL * tok[mine].astype(jnp.float32) + summed * dscale[...]
    mix_copy = pltpu.make_async_remote_copy(
        mixed.at[0], mixed.at[1], mix_sem.at[0], mix_sem.at[1], device_id={"cb": mate}, device_id_type=MESH
    )
    mix_copy.start()
    squares = jnp.sum(mixed[0] * mixed[0], axis=1, keepdims=True)
    spread[...] = jnp.zeros_like(spread)
    spread[mine] = jnp.broadcast_to(squares, (half, 128))
    out_own[...] = spread[...].T[:8]

    def out_copies():
        made = []
        for step in range(n):
            for other in range(2):
                if step or other:
                    at = 2 * step + other - 1
                    made.append(pltpu.make_async_remote_copy(
                        out_own, out_got.at[at], out_send.at[at], out_recv.at[at],
                        device_id={"ra": lax.rem(z + step, n), "cb": mate if other else cb},
                        device_id_type=MESH,
                    ))
        return made

    for copy in out_copies():
        copy.start()
    for copy in out_copies():
        copy.wait_recv()
    total = out_own[...]
    for at in range(2 * n - 1):
        total = total + out_got[at]
    spread[...] = jnp.broadcast_to(total[:1], (128, 128)).T
    spread[...] = lax.rsqrt(spread[...] / features + EPSILON)
    out_ref[mine] = (mixed[0] * spread[mine][:, :1] * ogain[...]).astype(jnp.bfloat16)
    mix_copy.wait()
    out_ref[theirs] = (mixed[1] * spread[theirs][:, :1] * ogain[...]).astype(jnp.bfloat16)

    for copy in out_copies():
        copy.wait_send()
    for goal, end in enumerate((0, n - 1)):
        @pl.when(z != end)
        def _():
            sq_copy(1, goal).wait_send()

    def drain(j, carry):
        @pl.when(z > 0)
        def _():
            rs_copy(j, 0).wait_send()
            ag_copy(j, 1).wait_send()

        @pl.when(z < n - 1)
        def _():
            rs_copy(j, 1).wait_send()
            ag_copy(j, 0).wait_send()

        return carry

    lax.fori_loop(0, chunks, drain, 0)


def fused(
    tokens, in_gain, gate_weight, gate_scale, up_weight, up_scale, down_weight, down_scale, out_gain
):
    n = lax.axis_size("ra")
    rows, depth = tokens.shape
    units, width = down_weight.shape
    half, chunks = rows // 2, units // WIDTH
    f32, bf16 = jnp.float32, jnp.bfloat16
    vmem, dma = pltpu.VMEM, pltpu.SemaphoreType.DMA
    return pl.pallas_call(
        functools.partial(kernel, n),
        out_shape=jax.ShapeDtypeStruct((rows, width), bf16),
        in_specs=[pl.BlockSpec(memory_space=pl.ANY)] * 9,
        out_specs=pl.BlockSpec(memory_space=pltpu.VMEM),
        scratch_shapes=[
            vmem((rows, depth), bf16), vmem((1, depth), f32),
            vmem((chunks, depth, WIDTH), f32), vmem((1, units), f32),
            vmem((chunks, depth, WIDTH), f32), vmem((1, units), f32),
            vmem((chunks, WIDTH, width), f32), vmem((1, width), f32), vmem((1, width), f32),
            vmem((rows, depth), bf16), vmem((chunks, rows, 2 * WIDTH), f32),
            vmem((2, chunks, half, 2 * WIDTH), bf16), vmem((2, chunks, half, 2 * WIDTH), bf16),
            vmem((chunks, rows, WIDTH), bf16), vmem((rows, width), f32),
            vmem((rows, 128), f32), vmem((1, 8, 128), f32), vmem((n - 1, 8, 128), f32),
            vmem((rows, 128), f32), vmem((half, width), bf16), vmem((half, width), bf16),
            vmem((half, width), bf16), vmem((half, width), bf16), vmem((2, half, width), f32),
            vmem((8, 128), f32), vmem((2 * n - 1, 8, 128), f32),
            dma((6,)), dma((chunks,)), dma((chunks,)), dma((chunks,)),
            dma((2, chunks)), dma((2, chunks)), dma((2, chunks)), dma((2, chunks)),
            dma((2,)), dma((n - 1,)), dma((2,)), dma((2,)), dma((2,)),
            dma((2 * n - 1,)), dma((2 * n - 1,)),
        ],
        compiler_params=pltpu.CompilerParams(
            collective_id=0, has_side_effects=True, vmem_limit_bytes=60 * 2**20
        ),
        name="fused_ffn",
    )(
        tokens, in_gain.reshape(1, -1), gate_weight, gate_scale.reshape(1, -1), up_weight,
        up_scale.reshape(1, -1), down_weight, down_scale.reshape(1, -1), out_gain.reshape(1, -1),
    )


def solution(mesh):
    in_specs = (
        P("grp", "ra"),
        P("ra"),
        P("ra", "cb"),
        P("cb"),
        P("ra", "cb"),
        P("cb"),
        P("cb", "ra"),
        P("ra"),
        P("ra"),
    )
    out_specs = P("grp", "ra")
    body = fused if mesh.shape["ra"] == 4 and mesh.shape["cb"] == 4 else local
    return jax.shard_map(body, mesh=mesh, in_specs=in_specs, out_specs=out_specs, check_vma=False)
```

```python
import functools
import jax
import jax.numpy as jnp
from jax import lax
from jax.experimental import pallas as pl
from jax.experimental.pallas import tpu as pltpu
from jax.sharding import PartitionSpec as P

EPSILON = 1e-06
RESIDUAL = 0.5


def local(
    tokens, in_gain, gate_weight, gate_scale, up_weight, up_scale, down_weight, down_scale, out_gain
):
    tok_float = tokens.astype(jnp.float32)
    local_squares = jnp.sum(tok_float * tok_float, axis=1)
    scaled = (tok_float * in_gain[None, :]).astype(jnp.bfloat16)
    gate_part = jnp.dot(
        scaled, gate_weight.astype(jnp.bfloat16), preferred_element_type=jnp.float32
    )
    up_part = jnp.dot(scaled, up_weight.astype(jnp.bfloat16), preferred_element_type=jnp.float32)
    features = tokens.shape[1] * lax.axis_size("ra")
    gate_sum, up_sum, share_squares = (
        lax.psum_scatter(gate_part, "ra", scatter_dimension=0, tiled=True),
        lax.psum_scatter(up_part, "ra", scatter_dimension=0, tiled=True),
        lax.psum_scatter(local_squares, "ra", scatter_dimension=0, tiled=True),
    )
    inv_rows = lax.rsqrt(share_squares / features + EPSILON)[:, None]
    gate_share = gate_sum * inv_rows * gate_scale[None, :]
    up_share = up_sum * inv_rows * up_scale[None, :]
    hidden_share = (jax.nn.silu(gate_share) * up_share).astype(jnp.bfloat16)
    hidden = lax.all_gather(hidden_share, "ra", axis=0, tiled=True)
    down_part = jnp.dot(
        hidden, down_weight.astype(jnp.bfloat16), preferred_element_type=jnp.float32
    )
    down_full = lax.psum(down_part, "cb")
    mixed_rows = RESIDUAL * tok_float + down_full * down_scale[None, :]
    out_total = lax.psum(jnp.sum(mixed_rows * mixed_rows, axis=1), "ra")
    inv_out = lax.rsqrt(out_total / features + EPSILON)[:, None]
    return (mixed_rows * inv_out * out_gain[None, :]).astype(jnp.bfloat16)


MESH = pl.DeviceIdType.MESH
WIDTH = 256
RS_LAG = 3
AG_LAG = 5
AHEAD = 3


def kernel(
    n,
    tok_hbm, gain_hbm, gate_hbm, gscale_hbm, up_hbm, uscale_hbm, down_hbm, dscale_hbm, ogain_hbm,
    out_ref,
    tok, gain, gate, gscale, up, uscale, down, dscale, ogain,
    scaled, part, sent, got, hidden, acc, spread, sq_own, sq_got, inv, half_sent, half_got,
    y_sent, y_got, mixed, out_own, out_got,
    small_sem, gate_sem, up_sem, down_sem, rs_send, rs_recv, ag_send, ag_recv,
    sq_send, sq_recv, half_sem, y_sem, mix_sem, out_send, out_recv,
):
    chunks, half = gate.shape[0], tok.shape[0] // 2
    rows = 2 * half
    features = tok.shape[1] * n
    z, cb = lax.axis_index("ra"), lax.axis_index("cb")
    core = lax.rem(cb, 2)
    mate = cb + 1 - 2 * core
    across = lax.rem(cb + 2, 4)
    right, left = lax.rem(z + 1, n), lax.rem(z + n - 1, n)

    smalls = [
        pltpu.make_async_copy(src, dst, small_sem.at[i])
        for i, (src, dst) in enumerate([
            (tok_hbm, tok), (gain_hbm, gain), (gscale_hbm, gscale),
            (uscale_hbm, uscale), (dscale_hbm, dscale), (ogain_hbm, ogain),
        ])
    ]

    def gate_copy(j):
        cols = pl.ds(pl.multiple_of(j * WIDTH, WIDTH), WIDTH)
        return pltpu.make_async_copy(gate_hbm.at[:, cols], gate.at[j], gate_sem.at[j])

    def up_copy(j):
        cols = pl.ds(pl.multiple_of(j * WIDTH, WIDTH), WIDTH)
        return pltpu.make_async_copy(up_hbm.at[:, cols], up.at[j], up_sem.at[j])

    def down_copy(j):
        at = pl.ds(pl.multiple_of(j * WIDTH, WIDTH), WIDTH)
        return pltpu.make_async_copy(down_hbm.at[at, :], down.at[j], down_sem.at[j])

    for copy in smalls:
        copy.start()
    for j in range(min(AHEAD, chunks)):
        gate_copy(j).start()
        up_copy(j).start()

    barrier = pltpu.get_barrier_semaphore()
    for step in range(1, n):
        for who in (cb, mate):
            pl.semaphore_signal(barrier, inc=1, device_id={"ra": lax.rem(z + step, n), "cb": who}, device_id_type=MESH)
    for who in (mate, across):
        pl.semaphore_signal(barrier, inc=1, device_id={"cb": who}, device_id_type=MESH)

    for copy in smalls:
        copy.wait()
    tok_float = tok[...].astype(jnp.float32)
    scaled[...] = (tok_float * gain[...]).astype(jnp.bfloat16)
    squares = jnp.sum(tok_float * tok_float, axis=1, keepdims=True)
    spread[...] = jnp.broadcast_to(squares, (rows, 128))
    sq_own[0] = spread[...].T[:8]

    pl.semaphore_wait(barrier, 2 * (n - 1) + 2)

    def sq_copy(step, goal):
        return pltpu.make_async_remote_copy(
            sq_own.at[0], sq_got.at[step - 1], sq_send.at[goal], sq_recv.at[step - 1],
            device_id={"ra": lax.rem(z + step, n)}, device_id_type=MESH,
        )

    for goal, end in enumerate((0, n - 1)):
        for step in range(1, n):
            @pl.when(lax.rem(z + step, n) == end)
            def _():
                sq_copy(step, goal).start()

    def rs_copy(j, side):
        return pltpu.make_async_remote_copy(
            sent.at[side, j], got.at[side, j], rs_send.at[side, j], rs_recv.at[side, j],
            device_id={"ra": right if side else left}, device_id_type=MESH,
        )

    def ag_copy(j, side):
        ref = hidden.at[j, pl.ds(side * half, half)]
        return pltpu.make_async_remote_copy(
            ref, ref, ag_send.at[side, j], ag_recv.at[side, j],
            device_id={"ra": left if side else right}, device_id_type=MESH,
        )

    def rs_step(t, side):
        place = z if side else n - 1 - z
        j = t - RS_LAG * place
        own = pl.ds(side * half, half)

        @pl.when((j >= 0) & (j < chunks))
        def _():
            @pl.when(place == 0)
            def _():
                sent[side, j] = part[j, own].astype(jnp.bfloat16)
                rs_copy(j, side).start()

            @pl.when((place > 0) & (place < n - 1))
            def _():
                rs_copy(j, side).wait_recv()
                sent[side, j] = (part[j, own] + got[side, j].astype(jnp.float32)).astype(jnp.bfloat16)
                rs_copy(j, side).start()

            @pl.when(place == n - 1)
            def _():
                @pl.when(j == 0)
                def _():
                    for step in range(1, n):
                        sq_copy(step, 0).wait_recv()
                    total = sq_own[0] + sq_got[0]
                    for step in range(2, n):
                        total = total + sq_got[step - 1]
                    spread[...] = jnp.broadcast_to(total[:1], (128, 128)).T
                    inv[...] = lax.rsqrt(spread[...] / features + EPSILON)

                rs_copy(j, side).wait_recv()
                scale = inv[own]
                total = part[j, own] + got[side, j].astype(jnp.float32)
                tiles = WIDTH // 128
                for i in range(tiles):
                    at, cols = pl.ds(j * tiles + i, 1), slice(128 * i, 128 * (i + 1))
                    gate_share = total[:, cols] * scale * gscale[at]
                    up_share = total[:, WIDTH:][:, cols] * scale * uscale[at]
                    hidden[j, own, cols] = (jax.nn.silu(gate_share) * up_share).astype(jnp.bfloat16)
                ag_copy(j, side).start()

    def rs_loop(t, carry):
        @pl.when(t < chunks)
        def _():
            gate_copy(t).wait()
            part[t, :, :WIDTH] = jnp.dot(scaled[...], gate[t].astype(jnp.bfloat16), preferred_element_type=jnp.float32)
            up_copy(t).wait()

            @pl.when(t + AHEAD < chunks)
            def _():
                gate_copy(t + AHEAD).start()
                up_copy(t + AHEAD).start()

            @pl.when(t == chunks - 1)
            def _():
                for j in range(chunks):
                    down_copy(j).start()

            part[t, :, WIDTH:] = jnp.dot(scaled[...], up[t].astype(jnp.bfloat16), preferred_element_type=jnp.float32)

        rs_step(t, 0)
        rs_step(t, 1)
        return carry

    lax.fori_loop(0, chunks + RS_LAG * (n - 1), rs_loop, 0)

    def ag_step(u, side):
        place = n - 1 - z if side else z
        j = u - AG_LAG * (place - 1)

        @pl.when((place > 0) & (j >= 0) & (j < chunks))
        def _():
            ag_copy(j, side).wait_recv()

            @pl.when(place < n - 1)
            def _():
                ag_copy(j, side).start()

    acc[...] = jnp.zeros_like(acc)

    def ag_loop(u, carry):
        ag_step(u, 0)
        ag_step(u, 1)
        j = u - AG_LAG * (lax.max(z, n - 1 - z) - 1)

        @pl.when((j >= 0) & (j < chunks))
        def _():
            down_copy(j).wait()
            acc[...] += jnp.dot(hidden[j], down[j].astype(jnp.bfloat16), preferred_element_type=jnp.float32)

        return carry

    lax.fori_loop(0, chunks + AG_LAG * (n - 2), ag_loop, 0)

    mine = pl.ds(pl.multiple_of(core * half, half), half)
    theirs = pl.ds(pl.multiple_of((1 - core) * half, half), half)
    half_sent[...] = acc[theirs].astype(jnp.bfloat16)
    half_copy = pltpu.make_async_remote_copy(
        half_sent, half_got, half_sem.at[0], half_sem.at[1], device_id={"cb": mate}, device_id_type=MESH
    )
    half_copy.start()
    half_copy.wait()
    y_sent[...] = (acc[mine] + half_got[...].astype(jnp.float32)).astype(jnp.bfloat16)
    y_copy = pltpu.make_async_remote_copy(
        y_sent, y_got, y_sem.at[0], y_sem.at[1], device_id={"cb": across}, device_id_type=MESH
    )
    y_copy.start()
    y_copy.wait()
    summed = y_sent[...].astype(jnp.float32) + y_got[...].astype(jnp.float32)
    mixed[0] = RESIDUAL * tok[mine].astype(jnp.float32) + summed * dscale[...]
    mix_copy = pltpu.make_async_remote_copy(
        mixed.at[0], mixed.at[1], mix_sem.at[0], mix_sem.at[1], device_id={"cb": mate}, device_id_type=MESH
    )
    mix_copy.start()
    squares = jnp.sum(mixed[0] * mixed[0], axis=1, keepdims=True)
    spread[...] = jnp.zeros_like(spread)
    spread[mine] = jnp.broadcast_to(squares, (half, 128))
    out_own[...] = spread[...].T[:8]

    def out_copies():
        made = []
        for step in range(n):
            for other in range(2):
                if step or other:
                    at = 2 * step + other - 1
                    made.append(pltpu.make_async_remote_copy(
                        out_own, out_got.at[at], out_send.at[at], out_recv.at[at],
                        device_id={"ra": lax.rem(z + step, n), "cb": mate if other else cb},
                        device_id_type=MESH,
                    ))
        return made

    for copy in out_copies():
        copy.start()
    for copy in out_copies():
        copy.wait_recv()
    total = out_own[...]
    for at in range(2 * n - 1):
        total = total + out_got[at]
    spread[...] = jnp.broadcast_to(total[:1], (128, 128)).T
    spread[...] = lax.rsqrt(spread[...] / features + EPSILON)
    out_ref[mine] = (mixed[0] * spread[mine][:, :1] * ogain[...]).astype(jnp.bfloat16)
    mix_copy.wait()
    out_ref[theirs] = (mixed[1] * spread[theirs][:, :1] * ogain[...]).astype(jnp.bfloat16)

    for copy in out_copies():
        copy.wait_send()
    for goal, end in enumerate((0, n - 1)):
        @pl.when(z != end)
        def _():
            sq_copy(1, goal).wait_send()

    def drain(j, carry):
        @pl.when(z > 0)
        def _():
            rs_copy(j, 0).wait_send()
            ag_copy(j, 1).wait_send()

        @pl.when(z < n - 1)
        def _():
            rs_copy(j, 1).wait_send()
            ag_copy(j, 0).wait_send()

        return carry

    lax.fori_loop(0, chunks, drain, 0)


def fused(
    tokens, in_gain, gate_weight, gate_scale, up_weight, up_scale, down_weight, down_scale, out_gain
):
    n = lax.axis_size("ra")
    rows, depth = tokens.shape
    units, width = down_weight.shape
    half, chunks = rows // 2, units // WIDTH
    f32, bf16 = jnp.float32, jnp.bfloat16
    vmem, dma = pltpu.VMEM, pltpu.SemaphoreType.DMA
    return pl.pallas_call(
        functools.partial(kernel, n),
        out_shape=jax.ShapeDtypeStruct((rows, width), bf16),
        in_specs=[pl.BlockSpec(memory_space=pl.ANY)] * 9,
        out_specs=pl.BlockSpec(memory_space=pltpu.VMEM),
        scratch_shapes=[
            vmem((rows, depth), bf16), vmem((1, depth), f32),
            vmem((chunks, depth, WIDTH), f32), vmem((units // 128, 128), f32),
            vmem((chunks, depth, WIDTH), f32), vmem((units // 128, 128), f32),
            vmem((chunks, WIDTH, width), f32), vmem((1, width), f32), vmem((1, width), f32),
            vmem((rows, depth), bf16), vmem((chunks, rows, 2 * WIDTH), f32),
            vmem((2, chunks, half, 2 * WIDTH), bf16), vmem((2, chunks, half, 2 * WIDTH), bf16),
            vmem((chunks, rows, WIDTH), bf16), vmem((rows, width), f32),
            vmem((rows, 128), f32), vmem((1, 8, 128), f32), vmem((n - 1, 8, 128), f32),
            vmem((rows, 128), f32), vmem((half, width), bf16), vmem((half, width), bf16),
            vmem((half, width), bf16), vmem((half, width), bf16), vmem((2, half, width), f32),
            vmem((8, 128), f32), vmem((2 * n - 1, 8, 128), f32),
            dma((6,)), dma((chunks,)), dma((chunks,)), dma((chunks,)),
            dma((2, chunks)), dma((2, chunks)), dma((2, chunks)), dma((2, chunks)),
            dma((2,)), dma((n - 1,)), dma((2,)), dma((2,)), dma((2,)),
            dma((2 * n - 1,)), dma((2 * n - 1,)),
        ],
        compiler_params=pltpu.CompilerParams(
            collective_id=0, has_side_effects=True, vmem_limit_bytes=60 * 2**20
        ),
        name="fused_ffn",
    )(
        tokens, in_gain.reshape(1, -1), gate_weight, gate_scale.reshape(-1, 128), up_weight,
        up_scale.reshape(-1, 128), down_weight, down_scale.reshape(1, -1), out_gain.reshape(1, -1),
    )


def solution(mesh):
    in_specs = (
        P("grp", "ra"),
        P("ra"),
        P("ra", "cb"),
        P("cb"),
        P("ra", "cb"),
        P("cb"),
        P("cb", "ra"),
        P("ra"),
        P("ra"),
    )
    out_specs = P("grp", "ra")
    body = fused if mesh.shape["ra"] == 4 and mesh.shape["cb"] == 4 else local
    return jax.shard_map(body, mesh=mesh, in_specs=in_specs, out_specs=out_specs, check_vma=False)
```
